32 devices in a mesh: fs: 8 (over z, core), tp: 4 (over y, x).
Axes of the slice: x: 2, y: 2, z: 4, core: 2. Of those that a mesh axis runs over, the one named last changes fastest.
Arguments:
- tokens: bfloat16 [1024, 2048], P('fs', 'tp'), may hold values from -6 to 6
- first_gain: float32 [2048], P('fs'), may hold values from 0.1 to 1.9
- first_gate: float32 [2048, 5504], P('fs', 'tp'), may hold values from -0.125 to 0.125
- first_up: float32 [2048, 5504], P('fs', 'tp'), may hold values from -0.125 to 0.125
- first_down: float32 [5504, 2048], P('tp', 'fs'), may hold values from -0.109375 to 0.109375
- first_post: float32 [2048], replicated, may hold values from 0.1 to 1.9
- second_gain: float32 [2048], P('fs'), may hold values from 0.1 to 1.9
- second_gate: float32 [2048, 5504], P('fs', 'tp'), may hold values from -0.125 to 0.125
- second_up: float32 [2048, 5504], P('fs', 'tp'), may hold values from -0.125 to 0.125
- second_down: float32 [5504, 2048], P('tp', 'fs'), may hold values from -0.109375 to 0.109375
- second_post: float32 [2048], replicated, may hold values from 0.1 to 1.9
Outputs:
- mixed: bfloat16 [1024, 2048], P('fs', 'tp')
- gate_one: bfloat16 [2048, 5504], P(None, 'tp')
- up_one: bfloat16 [2048, 5504], P(None, 'tp')
- down_one: bfloat16 [5504, 2048], P('tp')
- gate_two: bfloat16 [2048, 5504], P(None, 'tp')
- up_two: bfloat16 [2048, 5504], P(None, 'tp')
- down_two: bfloat16 [5504, 2048], P('tp')
The draws below stay inside these ranges and needn't reach their ends.
All inputs are finite; a program needn't handle non-finite values.
Results may differ from the reference program's by a relative error of at most 0.015.
Values may be sent and summed in bfloat16 or wider, within the bound.
A program may use at most 128 MiB of HBM per device.

```python
import jax
import jax.numpy as jnp
from jax import lax

D = 2048
FF = 5504
TOKENS = 1024
N_TP = 4


def spiked(result, own_key, source, target, shards_of, factor):
    def block_of(dim):
        return (jnp.arange(result.shape[dim]) // (result.shape[dim] // shards_of)).reshape((-1,) + (1,) * (result.ndim - 1 - dim))

    near = jax.random.permutation(own_key, shards_of)[block_of(target)]
    far = (block_of(target) + shards_of // 2) % shards_of
    return jnp.where((block_of(source) == near) | (block_of(source) == far), factor * result, result)


def level_of(own_key, shape, shards, least, top_value):
    def one(axis_at, parts):
        draws = jax.random.uniform(jax.random.fold_in(jax.random.fold_in(own_key, 6), axis_at), (parts,), jnp.float32, least / len(shards), top_value / len(shards))
        return jnp.repeat(jnp.exp(draws), shape[axis_at] // parts).reshape((-1,) + (1,) * (len(shape) - axis_at - 1))

    level = one(*shards[0])
    for cut in shards[1:]:
        level = level * one(*cut)
    return level


def centred(own_key, extent, deviation, most, pieces=(), held_as=jnp.bfloat16):
    loudness = level_of(own_key, extent, pieces, -0.22, 0.18) if pieces else 1.0
    entries = jax.random.normal(own_key, extent, jnp.float32) * deviation * loudness
    return jnp.minimum(jnp.maximum(entries, -most), most).astype(held_as)


def bell_draw_with(stream_key, dims, deviation, reach, split, heavy, kind=jnp.bfloat16):
    values = deviation * jax.random.normal(stream_key, dims, jnp.float32)
    if split:
        values = values * level_of(stream_key, dims, split, -0.22, 0.18)
    return jnp.clip(spiked(values, jax.random.fold_in(stream_key, 3), *heavy), -reach, reach).astype(kind)


def setup_inputs(seed: int = 0) -> dict:
    splits = jax.random.split(jax.random.key(seed), 12)
    tokens = centred(splits[0], (TOKENS, D), 1.0, 6.0, ((0, 8), (1, 4)))
    first_gain = jnp.clip(1.0 + 0.18 * jax.random.normal(splits[1], (D,), jnp.float32), 0.1, 1.9)
    first_gate = centred(splits[2], (D, FF), D ** -0.5, 0.125, ((0, 8), (1, 4)), jnp.float32)
    first_up = centred(splits[3], (D, FF), D ** -0.5, 0.125, ((0, 8), (1, 4)), jnp.float32)
    first_down = bell_draw_with(splits[4], (FF, D), FF ** -0.5, 0.109375, ((0, 4), (1, 8)), (0, 1, 8, 2.0), jnp.float32)
    first_post = jnp.clip(1.0 + 0.18 * jax.random.normal(splits[5], (D,), jnp.float32), 0.1, 1.9)
    second_gain = jnp.clip(1.0 + 0.18 * jax.random.normal(splits[6], (D,), jnp.float32), 0.1, 1.9)
    second_gate = centred(splits[7], (D, FF), D ** -0.5, 0.125, ((0, 8), (1, 4)), jnp.float32)
    second_up = centred(splits[8], (D, FF), D ** -0.5, 0.125, ((0, 8), (1, 4)), jnp.float32)
    second_down = bell_draw_with(splits[9], (FF, D), FF ** -0.5, 0.109375, ((0, 4), (1, 8)), (0, 1, 8, 2.0), jnp.float32)
    second_post = jnp.clip(1.0 + 0.18 * jax.random.normal(splits[10], (D,), jnp.float32), 0.1, 1.9)
    return dict(tokens=tokens, first_gain=first_gain, first_gate=first_gate, first_up=first_up, first_down=first_down, first_post=first_post, second_gain=second_gain, second_gate=second_gate, second_up=second_up, second_down=second_down, second_post=second_post)


norm_epsilon = 1e-06

def convert(gain, gate, up, down):
    gate_half = (gain[:, None] * gate).astype(jnp.bfloat16)
    up_half = (gain[:, None] * up).astype(jnp.bfloat16)
    return (gate_half, up_half, down.astype(jnp.bfloat16))

def half_step(rows, gate_w, up_w, down_w, post):
    rows_float = rows.astype(jnp.float32)
    scale = lax.rsqrt(lax.optimization_barrier(jnp.mean(rows_float * rows_float, axis=1, keepdims=True)) + norm_epsilon)
    gate = scale * jnp.dot(rows, gate_w, preferred_element_type=jnp.float32)
    up = scale * jnp.dot(rows, up_w, preferred_element_type=jnp.float32)
    hidden = (jax.nn.silu(gate) * up).astype(jnp.bfloat16)
    block = FF // N_TP

    def add_block(index, total):
        start = (index * block).astype(jnp.int32)
        piece = lax.dynamic_slice_in_dim(hidden, start, block, 1)
        weight = lax.dynamic_slice_in_dim(down_w, start, block, 0)
        part = jnp.dot(piece, weight, preferred_element_type=jnp.float32).astype(jnp.bfloat16)
        part = lax.optimization_barrier(part)
        return total + part.astype(jnp.float32)
    branch = lax.fori_loop(0, N_TP, add_block, jnp.zeros((rows.shape[0], D), jnp.float32))
    post_scale = lax.rsqrt(lax.optimization_barrier(jnp.mean(branch * branch, axis=1, keepdims=True)) + norm_epsilon)
    return (rows_float + 0.5 * branch * post_scale * post[None, :]).astype(jnp.bfloat16)

def reference(tokens, first_gain, first_gate, first_up, first_down, first_post, second_gain, second_gate, second_up, second_down, second_post):
    gate_one, up_one, down_one = convert(first_gain, first_gate, first_up, first_down)
    gate_two, up_two, down_two = convert(second_gain, second_gate, second_up, second_down)
    middle = half_step(tokens, gate_one, up_one, down_one, first_post)
    mixed = half_step(middle, gate_two, up_two, down_two, second_post)
    return (mixed, gate_one, up_one, down_one, gate_two, up_two, down_two)
```

```python
import jax
import jax.numpy as jnp
from jax import lax
from jax.sharding import PartitionSpec as P


norm_epsilon = 1e-06
CORES = 2
LINE = 4
MATRICES = 6


def after(value, *earlier):
    return lax.optimization_barrier((value, *earlier))[0]


def ring_parts(block_of, n_tp):
    me = lax.axis_index("tp")
    got = [block_of(me)]
    for d in range(1, n_tp):
        move = [(i, (i + d) % n_tp) for i in range(n_tp)]
        got.append(lax.ppermute(block_of((me + d) % n_tp), "tp", move))
    return got


def all_columns(columns, n_tp):
    me = lax.axis_index("tp")
    width = columns.shape[1]
    if n_tp > 8:
        return lax.all_gather(columns, "tp", axis=1, tiled=True)
    full = jnp.zeros((columns.shape[0], width * n_tp), columns.dtype)
    for d, block in enumerate(ring_parts(lambda _: columns, n_tp)):
        start = ((me - d + n_tp) % n_tp) * width
        full = lax.dynamic_update_slice_in_dim(full, block, start, 1)
    return full


def hidden_of(full_rows, gate_slab, up_slab):
    rows_float = full_rows.astype(jnp.float32)
    scale = lax.rsqrt(jnp.mean(rows_float * rows_float, axis=1, keepdims=True) + norm_epsilon)
    gate = scale * jnp.dot(full_rows, gate_slab, preferred_element_type=jnp.float32)
    up = scale * jnp.dot(full_rows, up_slab, preferred_element_type=jnp.float32)
    return (jax.nn.silu(gate) * up).astype(jnp.bfloat16)


def finish(own_columns, parts, post, n_tp):
    width = own_columns.shape[1]
    me = lax.axis_index("tp")
    features = width * n_tp
    if n_tp > 8:
        share = lax.psum_scatter(parts, "tp", scatter_dimension=1, tiled=True).astype(jnp.float32)
        squares = lax.psum(jnp.sum(share * share, axis=1, keepdims=True), "tp")
    else:
        got = ring_parts(lambda to: lax.dynamic_slice_in_dim(parts, to * width, width, 1), n_tp)
        share = got[0].astype(jnp.float32)
        for part in got[1:]:
            share = share + part.astype(jnp.float32)
        own = jnp.sum(share * share, axis=1)[None, :]
        sums = ring_parts(lambda _: own, n_tp)
        squares = sums[0]
        for one in sums[1:]:
            squares = squares + one
        squares = squares.reshape(-1, 1)
    scale = lax.rsqrt(squares / features + norm_epsilon)
    gain_part = lax.dynamic_slice_in_dim(post, me * width, width, 0)
    return (own_columns.astype(jnp.float32) + 0.5 * share * scale * gain_part[None, :]).astype(
        jnp.bfloat16
    )


def both_cores(pairs):
    return [(a * CORES + c, b * CORES + c) for a, b in pairs for c in range(CORES)]


def send(piece, pairs):
    return lax.ppermute(piece, "fs", both_cores(pairs))


def swap(piece):
    return lax.ppermute(piece, "fs", [(i, i ^ 1) for i in range(LINE * CORES)])


def put(slab, mine, other, chip, axis):
    core = lax.axis_index("fs") % CORES
    extent = mine.shape[axis]
    for piece, at in ((mine, core), (other, 1 - core)):
        slab = lax.dynamic_update_slice_in_dim(slab, piece, (chip * CORES + at) * extent, axis)
    return slab


def half(gain, gate, up, down):
    return (
        (gain[:, None] * gate).astype(jnp.bfloat16),
        (gain[:, None] * up).astype(jnp.bfloat16),
        down.astype(jnp.bfloat16),
    )


def line_program(n_tp):
    right = [(0, 1), (1, 2), (2, 3)]
    left = [(3, 2), (2, 1), (1, 0)]
    axes = (0, 0, 1) * 2

    def on_device(
        tokens,
        first_gain,
        first_gate,
        first_up,
        first_down,
        first_post,
        second_gain,
        second_gate,
        second_up,
        second_down,
        second_post,
    ):
        z = lax.axis_index("fs") // CORES
        low = z < LINE // 2
        outer = (z == 0) | (z == LINE - 1)
        far = LINE - 1 - z
        own = half(first_gain, first_gate, first_up, first_down)
        own = own + half(second_gain, second_gate, second_up, second_down)
        own = [lax.optimization_barrier(piece) for piece in own]

        from_left = [send(p, right) for p in own]
        from_right = [send(p, left) for p in own]
        from_left_two = [send(p, right[1:]) for p in from_left]
        from_right_two = [send(p, left[1:]) for p in from_right]
        across = [
            jnp.where(low, b, a) for a, b in zip(from_left_two, from_right_two)
        ]
        last = [send(p, [(1, 0), (2, 3)]) for p in across]

        neighbour = send(tokens, [(0, 1), (3, 2)])
        rows = jnp.concatenate([tokens, neighbour], axis=0)

        slabs = []
        for m, axis in enumerate(axes):
            piece = own[m]
            shape = list(piece.shape)
            shape[axis] *= LINE * CORES
            slab = jnp.broadcast_to(piece[:1, :1], tuple(shape))
            slab = put(slab, piece, swap(piece), z, axis)
            slab = put(slab, from_left[m], swap(from_left[m]), (z + LINE - 1) % LINE, axis)
            slab = put(slab, from_right[m], swap(from_right[m]), (z + 1) % LINE, axis)
            slab = put(slab, across[m], swap(across[m]), (z + LINE // 2) % LINE, axis)
            slabs.append(slab)

        def step(rows, gate, up, down, post):
            hidden = hidden_of(all_columns(rows, n_tp), gate, up)
            parts = jnp.dot(hidden, down, preferred_element_type=jnp.float32).astype(jnp.bfloat16)
            return finish(rows, parts, post, n_tp)

        middle = step(rows, *slabs[:3], first_post)
        both = mixed = step(middle, *slabs[3:], second_post)
        count = tokens.shape[0]
        back = send(mixed[count:], [(1, 0), (2, 3)])
        mixed = jnp.where(outer, back, mixed[:count])

        done, gates = [], [middle]
        for m, axis in enumerate(axes):
            if m == MATRICES // 2:
                gates.append(both)
            piece = jnp.where(outer, after(last[m], *gates), own[m])
            other = swap(piece)
            done.append(put(slabs[m], piece, other, jnp.where(outer, far, z), axis))
            gates = [other]
        return (mixed, *done)

    return on_device


def gathered_program(n_tp):
    def on_device(
        tokens,
        first_gain,
        first_gate,
        first_up,
        first_down,
        first_post,
        second_gain,
        second_gate,
        second_up,
        second_down,
        second_post,
    ):
        pieces = half(first_gain, first_gate, first_up, first_down)
        pieces = pieces + half(second_gain, second_gate, second_up, second_down)
        slabs = [
            lax.all_gather(piece, "fs", axis=axis, tiled=True)
            for piece, axis in zip(pieces, (0, 0, 1) * 2)
        ]
        rows = tokens
        for (gate, up, down), post in ((slabs[:3], first_post), (slabs[3:], second_post)):
            parts = jnp.dot(
                hidden_of(all_columns(rows, n_tp), gate, up),
                down,
                preferred_element_type=jnp.float32,
            ).astype(jnp.bfloat16)
            rows = finish(rows, parts, post, n_tp)
        return (rows, *slabs)

    return on_device


def solution(mesh):
    chips, n_tp = mesh.shape["fs"] // CORES, mesh.shape["tp"]
    program = line_program(n_tp) if chips == LINE else gathered_program(n_tp)

    placed = (
        P("fs", "tp"),
        P("fs"),
        P("fs", "tp"),
        P("fs", "tp"),
        P("tp", "fs"),
        P(),
        P("fs"),
        P("fs", "tp"),
        P("fs", "tp"),
        P("tp", "fs"),
        P(),
    )
    return jax.shard_map(
        program,
        mesh=mesh,
        in_specs=placed,
        out_specs=(
            P("fs", "tp"),
            P(None, "tp"),
            P(None, "tp"),
            P("tp", None),
            P(None, "tp"),
            P(None, "tp"),
            P("tp", None),
        ),
        check_vma=False,
    )
```

```python
import functools

import jax
import jax.numpy as jnp
from jax import lax
from jax.experimental import pallas as pl
from jax.experimental.pallas import tpu as pltpu
from jax.sharding import PartitionSpec as P

norm_epsilon = 1e-06
CORES = 2
LINE = 4
MATRICES = 6
LATE = 0
LANES = 128
MESH = pl.DeviceIdType.MESH
NT = (((1,), (1,)), ((), ()))


def half(gain, gate, up, down):
    return (
        (gain[:, None] * gate).astype(jnp.bfloat16),
        (gain[:, None] * up).astype(jnp.bfloat16),
        down.astype(jnp.bfloat16),
    )


def row_chunk(rows, most=64):
    fits = [c for c in range(16, most + 1, 16) if rows % c == 0]
    return fits[-1] if fits else rows


def line_kernel(
    n_tp,
    tokens,
    gains,
    posts,
    w0,
    w1,
    w2,
    w3,
    w4,
    w5,
    store,
    far,
    mixed,
    raw,
    own,
    held,
    rows,
    gate_sum,
    up_sum,
    hidden,
    parts,
    got,
    share,
    squares,
    result,
    load_sem,
    keep_sem,
    recv_sem,
    swap_sem,
    right_sem,
    left_sem,
    over_sem,
    held_sem,
    token_sem,
    row_send,
    row_recv,
    part_send,
    part_recv,
    square_send,
    square_recv,
    back_sem,
):
    fs, tp = lax.axis_index("fs"), lax.axis_index("tp")
    z, core = fs // CORES, lax.rem(fs, CORES)
    outer = (z == 0) | (z == LINE - 1)
    inner = jnp.logical_not(outer)
    low = z < LINE // 2
    weights = (w0, w1, w2, w3, w4, w5)
    height, width = w0.shape
    padded = held.shape[3]
    count, columns = tokens.shape
    features = columns * n_tp
    partner = (fs + 1 - 2 * core, tp)
    right, left = (fs + CORES, tp), (fs - CORES, tp)
    inward = (fs + jnp.where(low, CORES, -CORES), tp)
    outward = (fs + jnp.where(low, -CORES, CORES), tp)
    peers = [(fs, lax.rem(tp + d, n_tp)) for d in range(1, n_tp)]
    sources = [lax.rem(tp + n_tp - d, n_tp) for d in range(1, n_tp)]
    mine_at = pl.ds(pl.multiple_of(tp * columns, columns), columns)

    def home(m, rel):
        if rel == LINE // 2 and m >= MATRICES - LATE:
            return far.at[m - (MATRICES - LATE)]
        return store.at[m, rel, 0]

    def load(m):
        return pltpu.make_async_copy(weights[m], raw.at[m], load_sem.at[m])

    def keep(m):
        return pltpu.make_async_copy(own.at[m], store.at[m, 0, 0], keep_sem.at[m])

    def piece(m, rel):
        return own.at[m] if rel == 0 else home(m, rel)

    def to_right(m, rel):
        there = (rel + LINE - 1) % LINE
        return pltpu.make_async_remote_copy(
            piece(m, rel), home(m, there), right_sem.at[m, rel], recv_sem.at[m, there], right, MESH
        )

    def to_left(m, rel):
        there = rel + 1
        return pltpu.make_async_remote_copy(
            piece(m, rel), home(m, there), left_sem.at[m, rel], recv_sem.at[m, there], left, MESH
        )

    def over(m, rel):
        return pltpu.make_async_remote_copy(
            piece(m, rel), store.at[m, rel, 1], over_sem.at[m, rel], swap_sem.at[m, rel], partner, MESH
        )

    def arrived(m, rel):
        pltpu.make_async_copy(home(m, rel), home(m, rel), recv_sem.at[m, rel]).wait()

    def swapped(m, rel):
        here = store.at[m, rel, 1]
        pltpu.make_async_copy(here, here, swap_sem.at[m, rel]).wait()

    for m in range(MATRICES):
        load(m).start()

    token_in = pltpu.make_async_remote_copy(
        tokens, rows.at[0, pl.ds(count, count), mine_at], token_sem.at[0], token_sem.at[1], inward, MESH
    )
    token_own = pltpu.make_async_copy(tokens, rows.at[0, pl.ds(0, count), mine_at], token_sem.at[2])

    barrier = pltpu.get_barrier_semaphore()
    for peer in [partner, *peers]:
        pl.semaphore_signal(barrier, inc=1, device_id=peer, device_id_type=MESH)

    @pl.when(z > 0)
    def _():
        pl.semaphore_signal(barrier, inc=1, device_id=left, device_id_type=MESH)

    @pl.when(z < LINE - 1)
    def _():
        pl.semaphore_signal(barrier, inc=1, device_id=right, device_id_type=MESH)

    pl.semaphore_wait(barrier, n_tp + jnp.where(outer, 1, 2))

    chunk = row_chunk(height)
    for m in range(MATRICES):
        load(m).wait()
        if m % 3 == 2:

            def cast(i, _, m=m):
                at = pl.ds(pl.multiple_of(i * chunk, 16), chunk)
                own[m, at, :] = raw[m, at, :].astype(jnp.bfloat16)
                return 0
        else:

            def cast(i, _, m=m):
                at = pl.ds(pl.multiple_of(i * chunk, 16), chunk)
                own[m, at, :] = (gains[m // 3][None, :] * raw[m, at, :]).astype(jnp.bfloat16)
                return 0

        lax.fori_loop(0, height // chunk, cast, 0)

        @pl.when(z < LINE - 1)
        def _(m=m):
            to_right(m, 0).start()

        @pl.when(z > 0)
        def _(m=m):
            to_left(m, 0).start()

        over(m, 0).start()
        keep(m).start()
        if m == 0:

            @pl.when(outer)
            def _():
                token_in.start()

            @pl.when(inner)
            def _():
                token_own.start()

    def row_copy(step, d):
        block = rows.at[step, :, mine_at]
        return pltpu.make_async_remote_copy(
            block, block, row_send.at[step, d], row_recv.at[step, d], peers[d], MESH
        )

    def rows_in(step, d):
        at = pl.ds(pl.multiple_of(sources[d] * columns, columns), columns)
        block = rows.at[step, :, at]
        pltpu.make_async_copy(block, block, row_recv.at[step, d]).wait()

    @pl.when(inner)
    def _():
        token_own.wait()
        token_in.wait_recv()
        for d in range(n_tp - 1):
            row_copy(0, d).start()

    for m in range(MATRICES):

        @pl.when(z > 0)
        def _(m=m):
            arrived(m, LINE - 1)

            @pl.when(z < LINE - 1)
            def _():
                to_right(m, LINE - 1).start()

            over(m, LINE - 1).start()

        @pl.when(z < LINE - 1)
        def _(m=m):
            arrived(m, 1)

            @pl.when(z > 0)
            def _():
                to_left(m, 1).start()

            over(m, 1).start()

    for m in range(MATRICES):
        arrived(m, 2)
        if m < MATRICES - LATE:

            @pl.when(z == 1)
            def _(m=m):
                to_left(m, 2).start()

            @pl.when(z == 2)
            def _(m=m):
                to_right(m, 2).start()

        over(m, 2).start()

    def fetch(step, j, rel, c):
        m = step * 3 + j
        there = held.at[j, rel, c, pl.ds(0, height), :]
        here = home(m, rel) if c == 0 else store.at[m, rel, 1]
        return pltpu.make_async_copy(here, there, held_sem.at[step, j, rel, c])

    def feature_at(rel, c):
        source = lax.rem(z + rel, LINE) * CORES + (core if c == 0 else 1 - core)
        return pl.ds(pl.multiple_of(source * width, width), width)

    def part_copy(step, d):
        at = pl.ds(pl.multiple_of(peers[d][1] * columns, columns), columns)
        return pltpu.make_async_remote_copy(
            parts.at[step, :, at], got.at[step, d], part_send.at[step, d], part_recv.at[step, d], peers[d], MESH
        )

    def square_copy(step, d):
        return pltpu.make_async_remote_copy(
            squares.at[step, n_tp - 1],
            squares.at[step, d],
            square_send.at[step, d],
            square_recv.at[step, d],
            peers[d],
            MESH,
        )

    back = pltpu.make_async_remote_copy(
        result.at[pl.ds(count, count), :], mixed, back_sem.at[0], back_sem.at[1], outward, MESH
    )
    back_own = pltpu.make_async_copy(result.at[pl.ds(0, count), :], mixed, back_sem.at[2])
    both = 2 * count
    block = row_chunk(both, 32)

    @pl.when(inner)
    def _():
        for m in range(MATRICES):
            keep(m).wait()
            for rel in range(LINE):
                swapped(m, rel)
        for j in range(3):
            for rel in range(LINE):
                for c in range(CORES):
                    held[j, rel, c, pl.ds(height, padded - height), :] = jnp.zeros(
                        (padded - height, width), jnp.bfloat16
                    )
        for step in range(2):
            for j in range(3):
                for rel in range(LINE):
                    for c in range(CORES):
                        fetch(step, j, rel, c).start()
            for d in range(n_tp - 1):
                rows_in(step, d)
            for j in range(3):
                for rel in range(LINE):
                    for c in range(CORES):
                        fetch(step, j, rel, c).wait()

            gate_sum[...] = jnp.zeros_like(gate_sum)
            up_sum[...] = jnp.zeros_like(up_sum)

            def gate_up(rel, _, step=step):
                for c in range(CORES):
                    lhs = rows[step, :, feature_at(rel, c)]
                    for j, total in ((0, gate_sum), (1, up_sum)):
                        total[...] += lax.dot_general(
                            lhs, held[j, rel, c], NT, preferred_element_type=jnp.float32
                        )
                return 0

            lax.fori_loop(0, LINE, gate_up, 0)

            def activate(i, _, step=step):
                at = pl.ds(pl.multiple_of(i * block, 16), block)
                row = rows[step, at, :].astype(jnp.float32)
                scale = lax.rsqrt(
                    jnp.sum(row * row, axis=1, keepdims=True) / features + norm_epsilon
                )
                gate = scale * gate_sum[at, :]
                hidden[at, :] = (gate / (1.0 + jnp.exp(-gate)) * (scale * up_sum[at, :])).astype(
                    jnp.bfloat16
                )
                return 0

            lax.fori_loop(0, both // block, activate, 0)

            def down(rel, _, step=step):
                for c in range(CORES):
                    parts[step, :, feature_at(rel, c)] = jnp.dot(
                        hidden[...], held[2, rel, c], preferred_element_type=jnp.float32
                    ).astype(jnp.bfloat16)
                return 0

            lax.fori_loop(0, LINE, down, 0)
            for d in range(n_tp - 1):
                part_copy(step, d).start()
            for d in range(n_tp - 1):
                part_copy(step, d).wait_recv()

            def add_up(i, _, step=step):
                at = pl.ds(pl.multiple_of(i * block, 16), block)
                total = parts[step, at, mine_at].astype(jnp.float32)
                for d in range(n_tp - 1):
                    total = total + got[step, d, at, :].astype(jnp.float32)
                share[at, :] = total
                squares[step, n_tp - 1, at, :] = jnp.broadcast_to(
                    jnp.sum(total * total, axis=1, keepdims=True), (block, LANES)
                )
                return 0

            lax.fori_loop(0, both // block, add_up, 0)
            for d in range(n_tp - 1):
                square_copy(step, d).start()
            for d in range(n_tp - 1):
                square_copy(step, d).wait_recv()

            def finish(i, _, step=step):
                at = pl.ds(pl.multiple_of(i * block, 16), block)
                square = squares[step, n_tp - 1, at, :]
                for d in range(n_tp - 1):
                    square = square + squares[step, d, at, :]
                scale = lax.rsqrt(square[:, :1] / features + norm_epsilon)
                row = rows[step, at, mine_at].astype(jnp.float32)
                gain = posts[step, :, mine_at]
                out = (row + 0.5 * share[at, :] * scale * gain).astype(jnp.bfloat16)
                if step == 0:
                    rows[1, at, mine_at] = out
                else:
                    result[at, :] = out
                return 0

            lax.fori_loop(0, both // block, finish, 0)
            if step == 0:
                for d in range(n_tp - 1):
                    row_copy(1, d).start()
        back.start()
        back_own.start()

    @pl.when(outer)
    def _():
        for m in range(MATRICES - LATE):

            @pl.when(z == 0)
            def _(m=m):
                arrived(m, 3)
                over(m, 3).start()

            @pl.when(z == LINE - 1)
            def _(m=m):
                arrived(m, 1)
                over(m, 1).start()

        for m in range(MATRICES):
            keep(m).wait()
            swapped(m, 0)
            swapped(m, 2)

            @pl.when((z == 0) | (m < MATRICES - LATE))
            def _(m=m):
                swapped(m, 1)

            @pl.when((z == LINE - 1) | (m < MATRICES - LATE))
            def _(m=m):
                swapped(m, 3)

        back.wait_recv()
        token_in.wait_send()

    @pl.when(inner)
    def _():
        back.wait_send()
        back_own.wait()
        for step in range(2):
            for d in range(n_tp - 1):
                row_copy(step, d).wait_send()
                part_copy(step, d).wait_send()
                square_copy(step, d).wait_send()

    for m in range(MATRICES):
        over(m, 0).wait_send()
        over(m, 2).wait_send()
        late = m >= MATRICES - LATE

        @pl.when(z < LINE - 1)
        def _(m=m):
            to_right(m, 0).wait_send()
            over(m, 1).wait_send()

        @pl.when(z > 0)
        def _(m=m):
            to_left(m, 0).wait_send()
            over(m, 3).wait_send()

        @pl.when(inner)
        def _(m=m):
            to_right(m, 3).wait_send()
            to_left(m, 1).wait_send()

        if not late:

            @pl.when(z == 1)
            def _(m=m):
                to_left(m, 2).wait_send()

            @pl.when(z == 2)
            def _(m=m):
                to_right(m, 2).wait_send()

            @pl.when(z == 0)
            def _(m=m):
                over(m, 3).wait_send()

            @pl.when(z == LINE - 1)
            def _(m=m):
                over(m, 1).wait_send()


def gather_and_mix(n_tp, tokens, gains, posts, weights):
    height, width = weights[0].shape
    count, columns = tokens.shape
    features = columns * n_tp
    both = 2 * count
    padded = pl.cdiv(height, LANES) * LANES
    bf16, f32 = jnp.bfloat16, jnp.float32
    dma = pltpu.SemaphoreType.DMA
    others = n_tp - 1
    anywhere = pl.BlockSpec(memory_space=pl.ANY)
    vmem = pl.BlockSpec(memory_space=pltpu.VMEM)
    return pl.pallas_call(
        functools.partial(line_kernel, n_tp),
        out_shape=(
            jax.ShapeDtypeStruct((MATRICES, LINE, CORES, height, width), bf16),
            jax.ShapeDtypeStruct((max(LATE, 1), height, width), bf16),
            jax.ShapeDtypeStruct((count, columns), bf16),
        ),
        in_specs=[anywhere, vmem, vmem] + [anywhere] * MATRICES,
        out_specs=(anywhere, anywhere, anywhere),
        scratch_shapes=[
            pltpu.VMEM((MATRICES, height, width), f32),
            pltpu.VMEM((MATRICES, height, width), bf16),
            pltpu.VMEM((3, LINE, CORES, padded, width), bf16),
            pltpu.VMEM((2, both, features), bf16),
            pltpu.VMEM((both, padded), f32),
            pltpu.VMEM((both, padded), f32),
            pltpu.VMEM((both, padded), bf16),
            pltpu.VMEM((2, both, features), bf16),
            pltpu.VMEM((2, others, both, columns), bf16),
            pltpu.VMEM((both, columns), f32),
            pltpu.VMEM((2, n_tp, both, LANES), f32),
            pltpu.VMEM((both, columns), bf16),
            dma((MATRICES,)),
            dma((MATRICES,)),
            dma((MATRICES, LINE)),
            dma((MATRICES, LINE)),
            dma((MATRICES, LINE)),
            dma((MATRICES, LINE)),
            dma((MATRICES, LINE)),
            dma((2, 3, LINE, CORES)),
            dma((3,)),
            dma((2, others)),
            dma((2, others)),
            dma((2, others)),
            dma((2, others)),
            dma((2, others)),
            dma((2, others)),
            dma((3,)),
        ],
        compiler_params=pltpu.CompilerParams(
            collective_id=0, has_side_effects=True, vmem_limit_bytes=60 << 20
        ),
        cost_estimate=pl.CostEstimate(
            flops=200_000_000_000, bytes_accessed=100_000_000, transcendentals=0
        ),
        name="gather_and_mix",
    )(tokens, gains, posts, *weights)


def place_kernel(slots, store, *refs):
    outs, (held, in_sem, out_sem) = refs[:MATRICES], refs[MATRICES:]
    fs = lax.axis_index("fs")
    z, core = fs // CORES, lax.rem(fs, CORES)
    width = held.shape[2]
    jobs = [(m, rel, c) for m in range(MATRICES) for rel in range(LINE) for c in range(CORES)]

    def take(i):
        m, rel, c = jobs[i]
        return pltpu.make_async_copy(store.at[m, rel, c], held.at[i % slots], in_sem.at[i % slots])

    def give(i):
        m, rel, c = jobs[i]
        source = lax.rem(z + rel, LINE) * CORES + (core if c == 0 else 1 - core)
        at = pl.ds(pl.multiple_of(source * width, width), width)
        return pltpu.make_async_copy(held.at[i % slots], outs[m].at[:, at], out_sem.at[i % slots])

    lag = slots // 2
    for i in range(len(jobs) + lag):
        if i < len(jobs):
            if i >= slots:
                give(i - slots).wait()
            take(i).start()
        if i >= lag:
            take(i - lag).wait()
            give(i - lag).start()
    for i in range(len(jobs) - slots, len(jobs)):
        give(i).wait()


def place(store):
    height, width = store.shape[3:]
    slots = 16
    anywhere = pl.BlockSpec(memory_space=pl.ANY)
    return pl.pallas_call(
        functools.partial(place_kernel, slots),
        out_shape=(jax.ShapeDtypeStruct((height, width * LINE * CORES), jnp.bfloat16),) * MATRICES,
        in_specs=[anywhere],
        out_specs=(anywhere,) * MATRICES,
        scratch_shapes=[
            pltpu.VMEM((slots, height, width), jnp.bfloat16),
            pltpu.SemaphoreType.DMA((slots,)),
            pltpu.SemaphoreType.DMA((slots,)),
        ],
        compiler_params=pltpu.CompilerParams(vmem_limit_bytes=24 << 20),
        name="place",
    )(store)


def line_program(n_tp):
    def on_device(
        tokens,
        first_gain,
        first_gate,
        first_up,
        first_down,
        first_post,
        second_gain,
        second_gate,
        second_up,
        second_down,
        second_post,
    ):
        gains = jnp.stack([first_gain, second_gain])
        posts = jnp.stack([first_post, second_post])[:, None, :]
        weights = (first_gate.T, first_up.T, first_down, second_gate.T, second_up.T, second_down)
        store, far, mixed = gather_and_mix(n_tp, tokens, gains, posts, weights)
        slabs = place(store)
        return (
            mixed,
            slabs[0].T,
            slabs[1].T,
            slabs[2],
            slabs[3].T,
            slabs[4].T,
            slabs[5],
        )

    return on_device


def ring_parts(block_of, n_tp):
    me = lax.axis_index("tp")
    got = [block_of(me)]
    for d in range(1, n_tp):
        move = [(i, (i + d) % n_tp) for i in range(n_tp)]
        got.append(lax.ppermute(block_of((me + d) % n_tp), "tp", move))
    return got


def all_columns(columns, n_tp):
    me = lax.axis_index("tp")
    width = columns.shape[1]
    if n_tp > 8:
        return lax.all_gather(columns, "tp", axis=1, tiled=True)
    full = jnp.zeros((columns.shape[0], width * n_tp), columns.dtype)
    for d, block in enumerate(ring_parts(lambda _: columns, n_tp)):
        start = ((me - d + n_tp) % n_tp) * width
        full = lax.dynamic_update_slice_in_dim(full, block, start, 1)
    return full


def hidden_of(full_rows, gate_slab, up_slab):
    rows_float = full_rows.astype(jnp.float32)
    scale = lax.rsqrt(jnp.mean(rows_float * rows_float, axis=1, keepdims=True) + norm_epsilon)
    gate = scale * jnp.dot(full_rows, gate_slab, preferred_element_type=jnp.float32)
    up = scale * jnp.dot(full_rows, up_slab, preferred_element_type=jnp.float32)
    return (jax.nn.silu(gate) * up).astype(jnp.bfloat16)


def finish(own_columns, parts, post, n_tp):
    width = own_columns.shape[1]
    me = lax.axis_index("tp")
    features = width * n_tp
    if n_tp > 8:
        share = lax.psum_scatter(parts, "tp", scatter_dimension=1, tiled=True).astype(jnp.float32)
        squares = lax.psum(jnp.sum(share * share, axis=1, keepdims=True), "tp")
    else:
        got = ring_parts(lambda to: lax.dynamic_slice_in_dim(parts, to * width, width, 1), n_tp)
        share = got[0].astype(jnp.float32)
        for part in got[1:]:
            share = share + part.astype(jnp.float32)
        own = jnp.sum(share * share, axis=1)[None, :]
        sums = ring_parts(lambda _: own, n_tp)
        squares = sums[0]
        for one in sums[1:]:
            squares = squares + one
        squares = squares.reshape(-1, 1)
    scale = lax.rsqrt(squares / features + norm_epsilon)
    gain_part = lax.dynamic_slice_in_dim(post, me * width, width, 0)
    return (own_columns.astype(jnp.float32) + 0.5 * share * scale * gain_part[None, :]).astype(
        jnp.bfloat16
    )


def gathered_program(n_tp):
    def on_device(
        tokens,
        first_gain,
        first_gate,
        first_up,
        first_down,
        first_post,
        second_gain,
        second_gate,
        second_up,
        second_down,
        second_post,
    ):
        pieces = half(first_gain, first_gate, first_up, first_down)
        pieces = pieces + half(second_gain, second_gate, second_up, second_down)
        slabs = [
            lax.all_gather(piece, "fs", axis=axis, tiled=True)
            for piece, axis in zip(pieces, (0, 0, 1) * 2)
        ]
        rows = tokens
        for (gate, up, down), post in ((slabs[:3], first_post), (slabs[3:], second_post)):
            parts = jnp.dot(
                hidden_of(all_columns(rows, n_tp), gate, up),
                down,
                preferred_element_type=jnp.float32,
            ).astype(jnp.bfloat16)
            rows = finish(rows, parts, post, n_tp)
        return (rows, *slabs)

    return on_device


def solution(mesh):
    chips, n_tp = mesh.shape["fs"] // CORES, mesh.shape["tp"]
    program = line_program(n_tp) if chips == LINE else gathered_program(n_tp)

    placed = (
        P("fs", "tp"),
        P("fs"),
        P("fs", "tp"),
        P("fs", "tp"),
        P("tp", "fs"),
        P(),
        P("fs"),
        P("fs", "tp"),
        P("fs", "tp"),
        P("tp", "fs"),
        P(),
    )
    return jax.shard_map(
        program,
        mesh=mesh,
        in_specs=placed,
        out_specs=(
            P("fs", "tp"),
            P(None, "tp"),
            P(None, "tp"),
            P("tp", None),
            P(None, "tp"),
            P(None, "tp"),
            P("tp", None),
        ),
        check_vma=False,
    )
```

```python
import functools

import jax
import jax.numpy as jnp
from jax import lax
from jax.experimental import pallas as pl
from jax.experimental.pallas import tpu as pltpu
from jax.sharding import PartitionSpec as P


norm_epsilon = 1e-06
CORES = 2
LINE = 4
MATRICES = 6
LATE = 3
LANES = 128
MESH = pl.DeviceIdType.MESH


def half(gain, gate, up, down):
    return (
        (gain[:, None] * gate).astype(jnp.bfloat16),
        (gain[:, None] * up).astype(jnp.bfloat16),
        down.astype(jnp.bfloat16),
    )


def row_chunk(rows, most=64):
    fits = [c for c in range(16, most + 1, 16) if rows % c == 0]
    return fits[-1] if fits else rows


def line_kernel(
    n_tp,
    tokens,
    gain_one,
    gain_two,
    post_one,
    post_two,
    w0,
    w1,
    w2,
    w3,
    w4,
    w5,
    store,
    far_one,
    far_two,
    far_three,
    mixed,
    outgoing,
    raw,
    own,
    held,
    rows,
    turned,
    gate_sum,
    up_sum,
    hidden_turned,
    hidden,
    parts,
    got,
    share,
    squares,
    result,
    load_sem,
    keep_sem,
    recv_sem,
    swap_sem,
    right_sem,
    left_sem,
    over_sem,
    held_sem,
    token_sem,
    row_send,
    row_recv,
    part_send,
    part_recv,
    square_send,
    square_recv,
    back_sem,
):
    fs, tp = lax.axis_index("fs"), lax.axis_index("tp")
    z, core = fs // CORES, lax.rem(fs, CORES)
    outer = (z == 0) | (z == LINE - 1)
    inner = jnp.logical_not(outer)
    low = z < LINE // 2
    weights = (w0, w1, w2, w3, w4, w5)
    gains, posts, far = (gain_one, gain_two), (post_one, post_two), (far_one, far_two, far_three)
    height, width = w0.shape
    padded = held.shape[3]
    count, columns = tokens.shape
    features = columns * n_tp
    partner = (fs + 1 - 2 * core, tp)
    right, left = (fs + CORES, tp), (fs - CORES, tp)
    inward = (fs + jnp.where(low, CORES, -CORES), tp)
    peers = [(fs, lax.rem(tp + d, n_tp)) for d in range(1, n_tp)]
    sources = [lax.rem(tp + n_tp - d, n_tp) for d in range(1, n_tp)]
    mine_at = pl.ds(pl.multiple_of(tp * columns, columns), columns)

    def home(m, rel):
        if rel == LINE // 2 and m >= MATRICES - LATE:
            return far[m - (MATRICES - LATE)]
        return store.at[m, rel, 0]

    def load(m):
        return pltpu.make_async_copy(weights[m], raw.at[m], load_sem.at[m])

    def keep(m):
        return pltpu.make_async_copy(own.at[m], store.at[m, 0, 0], keep_sem.at[m])

    def piece(m, rel):
        return own.at[m] if rel == 0 else home(m, rel)

    def to_right(m, rel):
        there = (rel + LINE - 1) % LINE
        return pltpu.make_async_remote_copy(
            piece(m, rel), home(m, there), right_sem.at[m, rel], recv_sem.at[m, there], right, MESH
        )

    def to_left(m, rel):
        there = rel + 1
        return pltpu.make_async_remote_copy(
            piece(m, rel), home(m, there), left_sem.at[m, rel], recv_sem.at[m, there], left, MESH
        )

    def over(m, rel):
        return pltpu.make_async_remote_copy(
            piece(m, rel), store.at[m, rel, 1], over_sem.at[m, rel], swap_sem.at[m, rel], partner, MESH
        )

    def arrived(m, rel):
        pltpu.make_async_copy(home(m, rel), home(m, rel), recv_sem.at[m, rel]).wait()

    def swapped(m, rel):
        here = store.at[m, rel, 1]
        pltpu.make_async_copy(here, here, swap_sem.at[m, rel]).wait()

    for m in range(MATRICES):
        load(m).start()

    token_in = pltpu.make_async_remote_copy(
        tokens, rows.at[0, pl.ds(count, count), mine_at], token_sem.at[0], token_sem.at[1], inward, MESH
    )
    token_own = pltpu.make_async_copy(tokens, rows.at[0, pl.ds(0, count), mine_at], token_sem.at[2])

    barrier = pltpu.get_barrier_semaphore()
    for peer in [partner, *peers]:
        pl.semaphore_signal(barrier, inc=1, device_id=peer, device_id_type=MESH)

    @pl.when(z > 0)
    def _():
        pl.semaphore_signal(barrier, inc=1, device_id=left, device_id_type=MESH)

    @pl.when(z < LINE - 1)
    def _():
        pl.semaphore_signal(barrier, inc=1, device_id=right, device_id_type=MESH)

    pl.semaphore_wait(barrier, n_tp + jnp.where(outer, 1, 2))

    chunk = row_chunk(height)
    for m in range(MATRICES):
        load(m).wait()
        if m % 3 == 2:

            def cast(i, _, m=m):
                at = pl.ds(pl.multiple_of(i * chunk, 16), chunk)
                own[m, at, :] = raw[m, at, :].astype(jnp.bfloat16)
                return 0
        else:

            def cast(i, _, m=m):
                at = pl.ds(pl.multiple_of(i * chunk, 16), chunk)
                own[m, at, :] = (gains[m // 3][...] * raw[m, at, :]).astype(jnp.bfloat16)
                return 0

        lax.fori_loop(0, height // chunk, cast, 0)

        @pl.when(z < LINE - 1)
        def _(m=m):
            to_right(m, 0).start()

        @pl.when(z > 0)
        def _(m=m):
            to_left(m, 0).start()

        over(m, 0).start()
        keep(m).start()
        if m == 0:

            @pl.when(outer)
            def _():
                token_in.start()

            @pl.when(inner)
            def _():
                token_own.start()

    def row_copy(step, d):
        block = rows.at[step, :, mine_at]
        return pltpu.make_async_remote_copy(
            block, block, row_send.at[step, d], row_recv.at[step, d], peers[d], MESH
        )

    def rows_in(step, d):
        at = pl.ds(pl.multiple_of(sources[d] * columns, columns), columns)
        block = rows.at[step, :, at]
        pltpu.make_async_copy(block, block, row_recv.at[step, d]).wait()

    @pl.when(inner)
    def _():
        token_own.wait()
        token_in.wait_recv()
        for d in range(n_tp - 1):
            row_copy(0, d).start()

    for m in range(MATRICES):

        @pl.when(z > 0)
        def _(m=m):
            arrived(m, LINE - 1)

            @pl.when(z < LINE - 1)
            def _():
                to_right(m, LINE - 1).start()

            over(m, LINE - 1).start()

        @pl.when(z < LINE - 1)
        def _(m=m):
            arrived(m, 1)

            @pl.when(z > 0)
            def _():
                to_left(m, 1).start()

            over(m, 1).start()

    def fetch(step, j, rel, c):
        m = step * 3 + j
        there = held.at[j, rel, c, pl.ds(0, height), :]
        here = home(m, rel) if c == 0 else store.at[m, rel, 1]
        return pltpu.make_async_copy(here, there, held_sem.at[step, j, rel, c])

    def feature_at(rel, c):
        source = lax.rem(z + rel, LINE) * CORES + (core if c == 0 else 1 - core)
        return pl.ds(pl.multiple_of(source * width, width), width)

    def part_copy(step, d):
        at = pl.ds(pl.multiple_of(peers[d][1] * columns, columns), columns)
        return pltpu.make_async_remote_copy(
            parts.at[step, :, at], got.at[step, d], part_send.at[step, d], part_recv.at[step, d], peers[d], MESH
        )

    def square_copy(step, d):
        return pltpu.make_async_remote_copy(
            squares.at[step, n_tp - 1],
            squares.at[step, d],
            square_send.at[step, d],
            square_recv.at[step, d],
            peers[d],
            MESH,
        )

    results = [
        pltpu.make_async_copy(result.at[pl.ds(k * count, count), :], ref, back_sem.at[k])
        for k, ref in enumerate((mixed, outgoing))
    ]
    both = 2 * count
    block = row_chunk(both, 32)
    tall = row_chunk(padded, 64)

    def second(m):
        arrived(m, 2)
        if m < MATRICES - LATE:

            @pl.when(z == 1)
            def _():
                to_left(m, 2).start()

            @pl.when(z == 2)
            def _():
                to_right(m, 2).start()

        over(m, 2).start()

    @pl.when(outer)
    def _():
        for m in range(MATRICES):
            second(m)

    @pl.when(inner)
    def _():
        for j in range(3):
            for rel in range(LINE):
                for c in range(CORES):
                    held[j, rel, c, pl.ds(height, padded - height), :] = jnp.zeros(
                        (padded - height, width), jnp.bfloat16
                    )
        for step in range(2):
            for m in range(step * 3, step * 3 + 3):
                second(m)
            for m in range(step * 3, step * 3 + 3):
                keep(m).wait()
                for rel in range(LINE):
                    swapped(m, rel)
            for j in range(3):
                for rel in range(LINE):
                    for c in range(CORES):
                        fetch(step, j, rel, c).start()
            for d in range(n_tp - 1):
                rows_in(step, d)
            for j in range(3):
                for rel in range(LINE):
                    for c in range(CORES):
                        fetch(step, j, rel, c).wait()

            def turn(i, total, step=step):
                at = pl.ds(pl.multiple_of(i * width, width), width)
                flipped = rows[step, :, at].astype(jnp.float32).T
                turned[at, :] = flipped.astype(jnp.bfloat16)
                return total + jnp.sum(flipped * flipped, axis=0, keepdims=True)

            total = lax.fori_loop(
                0, features // width, turn, jnp.zeros((1, both), jnp.float32)
            )
            scale = lax.rsqrt(total / features + norm_epsilon)
            gate_sum[...] = jnp.zeros_like(gate_sum)
            up_sum[...] = jnp.zeros_like(up_sum)

            def gate_up(rel, _, step=step):
                for c in range(CORES):
                    rhs = turned[feature_at(rel, c), :]
                    for j, total in ((0, gate_sum), (1, up_sum)):
                        total[...] += jnp.dot(held[j, rel, c], rhs, preferred_element_type=jnp.float32)
                return 0

            lax.fori_loop(0, LINE, gate_up, 0)

            def activate(i, _, scale=scale):
                at = pl.ds(pl.multiple_of(i * tall, 16), tall)
                gate = scale * gate_sum[at, :]
                hidden_turned[at, :] = gate / (1.0 + jnp.exp(-gate)) * (scale * up_sum[at, :])
                return 0

            lax.fori_loop(0, padded // tall, activate, 0)

            def turn_back(i, _):
                at = pl.ds(pl.multiple_of(i * LANES, LANES), LANES)
                hidden[:, at] = hidden_turned[at, :].T.astype(jnp.bfloat16)
                return 0

            lax.fori_loop(0, padded // LANES, turn_back, 0)

            def down(rel, _, step=step):
                for c in range(CORES):
                    parts[step, :, feature_at(rel, c)] = jnp.dot(
                        hidden[...], held[2, rel, c], preferred_element_type=jnp.float32
                    ).astype(jnp.bfloat16)
                return 0

            lax.fori_loop(0, LINE, down, 0)
            for d in range(n_tp - 1):
                part_copy(step, d).start()
            for d in range(n_tp - 1):
                part_copy(step, d).wait_recv()

            def add_up(i, _, step=step):
                at = pl.ds(pl.multiple_of(i * block, 16), block)
                total = parts[step, at, mine_at].astype(jnp.float32)
                for d in range(n_tp - 1):
                    total = total + got[step, d, at, :].astype(jnp.float32)
                share[at, :] = total
                squares[step, n_tp - 1, at, :] = jnp.broadcast_to(
                    jnp.sum(total * total, axis=1, keepdims=True), (block, LANES)
                )
                return 0

            lax.fori_loop(0, both // block, add_up, 0)
            for d in range(n_tp - 1):
                square_copy(step, d).start()
            for d in range(n_tp - 1):
                square_copy(step, d).wait_recv()

            def finish(i, _, step=step):
                at = pl.ds(pl.multiple_of(i * block, 16), block)
                square = squares[step, n_tp - 1, at, :]
                for d in range(n_tp - 1):
                    square = square + squares[step, d, at, :]
                scale = lax.rsqrt(square[:, :1] / features + norm_epsilon)
                row = rows[step, at, mine_at].astype(jnp.float32)
                gain = posts[step][:, mine_at]
                out = (row + 0.5 * share[at, :] * scale * gain).astype(jnp.bfloat16)
                if step == 0:
                    rows[1, at, mine_at] = out
                else:
                    result[at, :] = out
                return 0

            lax.fori_loop(0, both // block, finish, 0)
            if step == 0:
                for d in range(n_tp - 1):
                    row_copy(1, d).start()
        for copy in results:
            copy.start()

    @pl.when(outer)
    def _():
        for m in range(MATRICES - LATE):

            @pl.when(z == 0)
            def _(m=m):
                arrived(m, 3)
                over(m, 3).start()

            @pl.when(z == LINE - 1)
            def _(m=m):
                arrived(m, 1)
                over(m, 1).start()

        for m in range(MATRICES):
            keep(m).wait()
            swapped(m, 0)
            swapped(m, 2)

            @pl.when((z == 0) | (m < MATRICES - LATE))
            def _(m=m):
                swapped(m, 1)

            @pl.when((z == LINE - 1) | (m < MATRICES - LATE))
            def _(m=m):
                swapped(m, 3)

        token_in.wait_send()

    @pl.when(inner)
    def _():
        for copy in results:
            copy.wait()
        for step in range(2):
            for d in range(n_tp - 1):
                row_copy(step, d).wait_send()
                part_copy(step, d).wait_send()
                square_copy(step, d).wait_send()

    for m in range(MATRICES):
        over(m, 0).wait_send()
        over(m, 2).wait_send()
        late = m >= MATRICES - LATE

        @pl.when(z < LINE - 1)
        def _(m=m):
            to_right(m, 0).wait_send()
            over(m, 1).wait_send()

        @pl.when(z > 0)
        def _(m=m):
            to_left(m, 0).wait_send()
            over(m, 3).wait_send()

        @pl.when(inner)
        def _(m=m):
            to_right(m, 3).wait_send()
            to_left(m, 1).wait_send()

        if not late:

            @pl.when(z == 1)
            def _(m=m):
                to_left(m, 2).wait_send()

            @pl.when(z == 2)
            def _(m=m):
                to_right(m, 2).wait_send()

            @pl.when(z == 0)
            def _(m=m):
                over(m, 3).wait_send()

            @pl.when(z == LINE - 1)
            def _(m=m):
                over(m, 1).wait_send()


def gather_and_mix(n_tp, tokens, gains, posts, weights):
    height, width = weights[0].shape
    count, columns = tokens.shape
    features = columns * n_tp
    both = 2 * count
    padded = pl.cdiv(height, LANES) * LANES
    bf16, f32 = jnp.bfloat16, jnp.float32
    dma = pltpu.SemaphoreType.DMA
    others = n_tp - 1
    anywhere = pl.BlockSpec(memory_space=pl.ANY)
    vmem = pl.BlockSpec(memory_space=pltpu.VMEM)
    return pl.pallas_call(
        functools.partial(line_kernel, n_tp),
        out_shape=(
            jax.ShapeDtypeStruct((MATRICES, LINE, CORES, height, width), bf16),
            *(jax.ShapeDtypeStruct((height, width), bf16),) * LATE,
            *(jax.ShapeDtypeStruct((count, columns), bf16),) * 2,
        ),
        in_specs=[anywhere] + [vmem] * 4 + [anywhere] * MATRICES,
        out_specs=(anywhere,) * (LATE + 3),
        scratch_shapes=[
            pltpu.VMEM((MATRICES, height, width), f32),
            pltpu.VMEM((MATRICES, height, width), bf16),
            pltpu.VMEM((3, LINE, CORES, padded, width), bf16),
            pltpu.VMEM((2, both, features), bf16),
            pltpu.VMEM((features, both), bf16),
            pltpu.VMEM((padded, both), f32),
            pltpu.VMEM((padded, both), f32),
            pltpu.VMEM((padded, both), f32),
            pltpu.VMEM((both, padded), bf16),
            pltpu.VMEM((2, both, features), bf16),
            pltpu.VMEM((2, others, both, columns), bf16),
            pltpu.VMEM((both, columns), f32),
            pltpu.VMEM((2, n_tp, both, LANES), f32),
            pltpu.VMEM((both, columns), bf16),
            dma((MATRICES,)),
            dma((MATRICES,)),
            dma((MATRICES, LINE)),
            dma((MATRICES, LINE)),
            dma((MATRICES, LINE)),
            dma((MATRICES, LINE)),
            dma((MATRICES, LINE)),
            dma((2, 3, LINE, CORES)),
            dma((3,)),
            dma((2, others)),
            dma((2, others)),
            dma((2, others)),
            dma((2, others)),
            dma((2, others)),
            dma((2, others)),
            dma((2,)),
        ],
        compiler_params=pltpu.CompilerParams(
            collective_id=0, has_side_effects=True, vmem_limit_bytes=60 << 20
        ),
        cost_estimate=pl.CostEstimate(
            flops=200_000_000_000, bytes_accessed=100_000_000, transcendentals=0
        ),
        name="gather_and_mix",
    )(tokens, *gains, *posts, *weights)


def place_kernel(slots, store, *refs):
    far, outs = refs[:LATE], refs[LATE : LATE + MATRICES]
    held, in_sem, out_sem = refs[LATE + MATRICES :]
    fs = lax.axis_index("fs")
    z, core = fs // CORES, lax.rem(fs, CORES)
    width = held.shape[2]
    jobs = [(m, rel, c) for m in range(MATRICES) for rel in range(LINE) for c in range(CORES)]

    def take(i):
        m, rel, c = jobs[i]
        late = m - (MATRICES - LATE)
        piece = far[late] if rel == LINE // 2 and c == 0 and late >= 0 else store.at[m, rel, c]
        return pltpu.make_async_copy(piece, held.at[i % slots], in_sem.at[i % slots])

    def give(i):
        m, rel, c = jobs[i]
        source = lax.rem(z + rel, LINE) * CORES + (core if c == 0 else 1 - core)
        at = pl.ds(pl.multiple_of(source * width, width), width)
        return pltpu.make_async_copy(held.at[i % slots], outs[m].at[:, at], out_sem.at[i % slots])

    lag = slots // 2
    for i in range(len(jobs) + lag):
        if i < len(jobs):
            if i >= slots:
                give(i - slots).wait()
            take(i).start()
        if i >= lag:
            take(i - lag).wait()
            give(i - lag).start()
    for i in range(len(jobs) - slots, len(jobs)):
        give(i).wait()


def place(store, far):
    height, width = store.shape[3:]
    slots = 16
    anywhere = pl.BlockSpec(memory_space=pltpu.HBM)
    slab = jax.ShapeDtypeStruct((height, width * LINE * CORES), jnp.bfloat16)
    return pl.pallas_call(
        functools.partial(place_kernel, slots),
        out_shape=(slab,) * MATRICES,
        in_specs=[anywhere] * (LATE + 1),
        out_specs=(anywhere,) * MATRICES,
        scratch_shapes=[
            pltpu.VMEM((slots, height, width), jnp.bfloat16),
            pltpu.SemaphoreType.DMA((slots,)),
            pltpu.SemaphoreType.DMA((slots,)),
        ],
        compiler_params=pltpu.CompilerParams(vmem_limit_bytes=24 << 20),
        cost_estimate=pl.CostEstimate(
            flops=20_000_000_000, bytes_accessed=68_000_000, transcendentals=0
        ),
        name="place",
    )(store, *far)


def put_kernel(first, slab_in, mine, other, slab, held, sems):
    fs = lax.axis_index("fs")
    z, core = fs // CORES, lax.rem(fs, CORES)
    height, width = mine.shape
    copies = []
    for c, piece in enumerate((mine, other)):
        source = (LINE - 1 - z) * CORES + (core if c == 0 else 1 - core)
        at = pl.ds(pl.multiple_of(source * width, width), width)
        copies.append(
            (
                pltpu.make_async_copy(piece, held.at[c], sems.at[c, 0]),
                pltpu.make_async_copy(held.at[c], slab.at[pl.ds(first, height), at], sems.at[c, 1]),
            )
        )

    @pl.when((z == 0) | (z == LINE - 1))
    def _():
        for take, _ in copies:
            take.start()
        for take, give in copies:
            take.wait()
            give.start()
        for _, give in copies:
            give.wait()


def put(slab, mine, other, first):
    anywhere = pl.BlockSpec(memory_space=pl.ANY)
    return pl.pallas_call(
        functools.partial(put_kernel, first),
        out_shape=jax.ShapeDtypeStruct(slab.shape, slab.dtype),
        in_specs=[anywhere] * 3,
        out_specs=anywhere,
        scratch_shapes=[
            pltpu.VMEM((CORES, *mine.shape), mine.dtype),
            pltpu.SemaphoreType.DMA((CORES, 2)),
        ],
        input_output_aliases={0: 0},
        compiler_params=pltpu.CompilerParams(vmem_limit_bytes=4 << 20),
        cost_estimate=pl.CostEstimate(
            flops=1_000_000_000, bytes_accessed=3_000_000, transcendentals=0
        ),
        name="put",
    )(slab, mine, other)


def hop(piece):
    pairs = [(a * CORES + c, b * CORES + c) for a, b in ((1, 0), (2, 3)) for c in range(CORES)]
    return lax.ppermute(piece, "fs", pairs)


def swap(piece):
    pairs = [(z * CORES + c, z * CORES + 1 - c) for z in (0, LINE - 1) for c in range(CORES)]
    return lax.ppermute(piece, "fs", pairs)


def line_program(n_tp):
    def on_device(
        tokens,
        first_gain,
        first_gate,
        first_up,
        first_down,
        first_post,
        second_gain,
        second_gate,
        second_up,
        second_down,
        second_post,
    ):
        gains = (first_gain[None, :], second_gain[None, :])
        posts = (first_post[None, :], second_post[None, :])
        weights = (first_gate.T, first_up.T, first_down, second_gate.T, second_up.T, second_down)
        store, *far, mixed, outgoing = gather_and_mix(n_tp, tokens, gains, posts, weights)
        height = far[0].shape[0]
        cut = height // 2 // 16 * 16
        late = [(k, far[k], 0) for k in range(LATE - 1)]
        late += [(LATE - 1, far[-1][:cut], 0), (LATE - 1, far[-1][cut:], cut)]
        moved = [hop(piece) for _, piece, _ in late]
        back = hop(outgoing)
        slabs = list(place(store, far))
        for i, (k, _, first) in enumerate(late):
            m = MATRICES - LATE + k
            other = swap(moved[i])
            slabs[m] = put(slabs[m], moved[i], other, first)
        z = lax.axis_index("fs") // CORES
        mixed = jnp.where((z == 0) | (z == LINE - 1), back, mixed)
        return (
            mixed,
            slabs[0].T,
            slabs[1].T,
            slabs[2],
            slabs[3].T,
            slabs[4].T,
            slabs[5],
        )

    return on_device


def ring_parts(block_of, n_tp):
    me = lax.axis_index("tp")
    got = [block_of(me)]
    for d in range(1, n_tp):
        move = [(i, (i + d) % n_tp) for i in range(n_tp)]
        got.append(lax.ppermute(block_of((me + d) % n_tp), "tp", move))
    return got


def all_columns(columns, n_tp):
    me = lax.axis_index("tp")
    width = columns.shape[1]
    if n_tp > 8:
        return lax.all_gather(columns, "tp", axis=1, tiled=True)
    full = jnp.zeros((columns.shape[0], width * n_tp), columns.dtype)
    for d, block in enumerate(ring_parts(lambda _: columns, n_tp)):
        start = ((me - d + n_tp) % n_tp) * width
        full = lax.dynamic_update_slice_in_dim(full, block, start, 1)
    return full


def hidden_of(full_rows, gate_slab, up_slab):
    rows_float = full_rows.astype(jnp.float32)
    scale = lax.rsqrt(jnp.mean(rows_float * rows_float, axis=1, keepdims=True) + norm_epsilon)
    gate = scale * jnp.dot(full_rows, gate_slab, preferred_element_type=jnp.float32)
    up = scale * jnp.dot(full_rows, up_slab, preferred_element_type=jnp.float32)
    return (jax.nn.silu(gate) * up).astype(jnp.bfloat16)


def finish(own_columns, parts, post, n_tp):
    width = own_columns.shape[1]
    me = lax.axis_index("tp")
    features = width * n_tp
    if n_tp > 8:
        share = lax.psum_scatter(parts, "tp", scatter_dimension=1, tiled=True).astype(jnp.float32)
        squares = lax.psum(jnp.sum(share * share, axis=1, keepdims=True), "tp")
    else:
        got = ring_parts(lambda to: lax.dynamic_slice_in_dim(parts, to * width, width, 1), n_tp)
        share = got[0].astype(jnp.float32)
        for part in got[1:]:
            share = share + part.astype(jnp.float32)
        own = jnp.sum(share * share, axis=1)[None, :]
        sums = ring_parts(lambda _: own, n_tp)
        squares = sums[0]
        for one in sums[1:]:
            squares = squares + one
        squares = squares.reshape(-1, 1)
    scale = lax.rsqrt(squares / features + norm_epsilon)
    gain_part = lax.dynamic_slice_in_dim(post, me * width, width, 0)
    return (own_columns.astype(jnp.float32) + 0.5 * share * scale * gain_part[None, :]).astype(
        jnp.bfloat16
    )


def gathered_program(n_tp):
    def on_device(
        tokens,
        first_gain,
        first_gate,
        first_up,
        first_down,
        first_post,
        second_gain,
        second_gate,
        second_up,
        second_down,
        second_post,
    ):
        pieces = half(first_gain, first_gate, first_up, first_down)
        pieces = pieces + half(second_gain, second_gate, second_up, second_down)
        slabs = [
            lax.all_gather(piece, "fs", axis=axis, tiled=True)
            for piece, axis in zip(pieces, (0, 0, 1) * 2)
        ]
        rows = tokens
        for (gate, up, down), post in ((slabs[:3], first_post), (slabs[3:], second_post)):
            parts = jnp.dot(
                hidden_of(all_columns(rows, n_tp), gate, up),
                down,
                preferred_element_type=jnp.float32,
            ).astype(jnp.bfloat16)
            rows = finish(rows, parts, post, n_tp)
        return (rows, *slabs)

    return on_device


def solution(mesh):
    chips, n_tp = mesh.shape["fs"] // CORES, mesh.shape["tp"]
    program = line_program(n_tp) if chips == LINE else gathered_program(n_tp)

    placed = (
        P("fs", "tp"),
        P("fs"),
        P("fs", "tp"),
        P("fs", "tp"),
        P("tp", "fs"),
        P(),
        P("fs"),
        P("fs", "tp"),
        P("fs", "tp"),
        P("tp", "fs"),
        P(),
    )

    return jax.shard_map(
        program,
        mesh=mesh,
        in_specs=placed,
        out_specs=(
            P("fs", "tp"),
            P(None, "tp"),
            P(None, "tp"),
            P("tp", None),
            P(None, "tp"),
            P(None, "tp"),
            P("tp", None),
        ),
        check_vma=False,
    )
```

```python
import functools

import jax
import jax.numpy as jnp
from jax import lax
from jax.experimental import pallas as pl
from jax.experimental.pallas import tpu as pltpu
from jax.sharding import PartitionSpec as P


norm_epsilon = 1e-06
CORES = 2
LINE = 4
MATRICES = 6
LATE = 4
MOVES = 3
EDGE = MATRICES - LATE
INNER = EDGE - 1
FIRST = 4
LANES = 128
SUBLANES = 8
SLOTS = 3
MESH = pl.DeviceIdType.MESH


def half(gain, gate, up, down):
    return (
        (gain[:, None] * gate).astype(jnp.bfloat16),
        (gain[:, None] * up).astype(jnp.bfloat16),
        down.astype(jnp.bfloat16),
    )


def row_chunk(rows, most=64):
    fits = [c for c in range(16, most + 1, 16) if rows % c == 0]
    return fits[-1] if fits else rows


def line_kernel(
    n_tp,
    tokens,
    gain_one,
    gain_two,
    post_one,
    post_two,
    w0,
    w1,
    w2,
    w3,
    w4,
    w5,
    store,
    far_first,
    far_pair,
    far_last,
    tail,
    edge,
    mixed,
    outgoing,
    raw,
    own,
    held,
    rows,
    column,
    gate_sum,
    up_sum,
    hidden_turned,
    hidden,
    parts,
    got,
    share,
    squares,
    result,
    go_sem,
    load_sem,
    keep_sem,
    recv_sem,
    swap_sem,
    right_sem,
    left_sem,
    over_sem,
    held_sem,
    token_sem,
    row_send,
    row_recv,
    part_send,
    part_recv,
    square_send,
    square_recv,
    back_sem,
):
    fs, tp = lax.axis_index("fs"), lax.axis_index("tp")
    z, core = fs // CORES, lax.rem(fs, CORES)
    outer = (z == 0) | (z == LINE - 1)
    inner = jnp.logical_not(outer)
    low = z < LINE // 2
    weights = (w0, w1, w2, w3, w4, w5)
    gains, posts = (gain_one, gain_two), (post_one, post_two)
    height, width = w0.shape
    lower, upper = pl.ds(0, height), pl.ds(height, height)
    cut = edge.shape[0] - height
    far = dict(
        zip(
            range(EDGE, MATRICES),
            (far_first, far_pair.at[lower], far_pair.at[upper], far_last),
        )
    )
    edges = {INNER: edge.at[lower], EDGE: edge.at[pl.ds(height, cut)]}
    padded = held.shape[3]
    count, columns = tokens.shape
    features = columns * n_tp
    partner = (fs + 1 - 2 * core, tp)
    right, left = (fs + CORES, tp), (fs - CORES, tp)
    inward = (fs + jnp.where(low, CORES, -CORES), tp)
    peers = [(fs, lax.rem(tp + d, n_tp)) for d in range(1, n_tp)]
    sources = [lax.rem(tp + n_tp - d, n_tp) for d in range(1, n_tp)]
    mine_at = pl.ds(pl.multiple_of(tp * columns, columns), columns)

    def home(m, rel):
        if rel == LINE // 2 and m in far:
            return far[m]
        return store.at[m, rel, 0]

    def landing(m, rel):
        return edges.get(m) if m in edges else home(m, rel)

    def load(m):
        return pltpu.make_async_copy(weights[m], raw.at[m % SLOTS], load_sem.at[m])

    def keep(m):
        return pltpu.make_async_copy(own.at[m], store.at[m, 0, 0], keep_sem.at[m])

    def piece(m, rel):
        return own.at[m] if rel == 0 else home(m, rel)

    def send(m, rel, there, sem, target, at):
        end = landing if rel == LINE // 2 else home
        return pltpu.make_async_remote_copy(
            piece(m, rel).at[at],
            end(m, there).at[at],
            sem.at[m, rel],
            recv_sem.at[m, there],
            target,
            MESH,
        )

    whole = pl.ds(0, height)
    early = pl.ds(0, cut)

    def to_right(m, rel, at=whole):
        return send(m, rel, (rel + LINE - 1) % LINE, right_sem, right, at)

    def to_left(m, rel, at=whole):
        return send(m, rel, rel + 1, left_sem, left, at)

    def over(m, rel):
        return pltpu.make_async_remote_copy(
            piece(m, rel), store.at[m, rel, 1], over_sem.at[m, rel], swap_sem.at[m, rel], partner, MESH
        )

    def arrived(m, rel):
        pltpu.make_async_copy(home(m, rel), home(m, rel), recv_sem.at[m, rel]).wait()

    def arrived_last(m, rel):
        here = landing(m, rel)
        pltpu.make_async_copy(here, here, recv_sem.at[m, rel]).wait()

    def swapped(m, rel):
        here = store.at[m, rel, 1]
        pltpu.make_async_copy(here, here, swap_sem.at[m, rel]).wait()

    load(0).start()

    token_in = pltpu.make_async_remote_copy(
        tokens, rows.at[0, pl.ds(count, count), mine_at], token_sem.at[0], token_sem.at[1], inward, MESH
    )
    token_own = pltpu.make_async_copy(tokens, rows.at[0, pl.ds(0, count), mine_at], token_sem.at[2])

    barrier = pltpu.get_barrier_semaphore()
    for peer in [partner, *peers]:
        pl.semaphore_signal(barrier, inc=1, device_id=peer, device_id_type=MESH)

    @pl.when(z > 0)
    def _():
        pl.semaphore_signal(barrier, inc=1, device_id=left, device_id_type=MESH)

    @pl.when(z < LINE - 1)
    def _():
        pl.semaphore_signal(barrier, inc=1, device_id=right, device_id_type=MESH)

    def cast(m, at):
        value = raw[m % SLOTS, at, :]
        if m % 3 != 2:
            value = gains[m // 3][...] * value
        own[m, at, :] = value.astype(jnp.bfloat16)

    def first_hops(m, at):
        @pl.when(z < LINE - 1)
        def _():
            to_right(m, 0, at).start()

        @pl.when(z > 0)
        def _():
            to_left(m, 0, at).start()

    load(0).wait()
    for m in range(1, SLOTS):
        load(m).start()
    for m in range(MATRICES):
        if m > 0:
            load(m).wait()
        cuts = FIRST if m == 0 and height % (16 * FIRST) == 0 else 1
        size = height // cuts
        chunk = row_chunk(size)
        for q in range(cuts):

            def cast_chunk(i, _, m=m, q=q, size=size, chunk=chunk):
                cast(m, pl.ds(pl.multiple_of(q * size + i * chunk, 16), chunk))
                return 0

            lax.fori_loop(0, size // chunk, cast_chunk, 0)
            at = pl.ds(q * size, size)
            if m == 0 and q == 0:
                pl.semaphore_wait(barrier, n_tp + jnp.where(outer, 1, 2))

            @pl.when(core == 0)
            def _(m=m, at=at):
                first_hops(m, at)

        over(m, 0).start()
        keep(m).start()
        if m + SLOTS < MATRICES:
            load(m + SLOTS).start()
        if m == 0:

            @pl.when(outer)
            def _():
                token_in.start()

            @pl.when(inner)
            def _():
                token_own.start()

    @pl.when(core == 1)
    def _():
        pl.semaphore_wait(go_sem, 1)
        for m in range(MATRICES):
            first_hops(m, whole)

    def row_copy(step, d):
        block = rows.at[step, :, mine_at]
        return pltpu.make_async_remote_copy(
            block, block, row_send.at[step, d], row_recv.at[step, d], peers[d], MESH
        )

    def rows_in(step, d):
        at = pl.ds(pl.multiple_of(sources[d] * columns, columns), columns)
        block = rows.at[step, :, at]
        pltpu.make_async_copy(block, block, row_recv.at[step, d]).wait()

    @pl.when(inner)
    def _():
        token_own.wait()
        token_in.wait_recv()
        for d in range(n_tp - 1):
            row_copy(0, d).start()

    for m in range(MATRICES):
        if m == 1:

            @pl.when(core == 0)
            def _():
                pl.semaphore_signal(go_sem, inc=1, device_id=partner, device_id_type=MESH)

        @pl.when(z > 0)
        def _(m=m):
            arrived(m, LINE - 1)

            @pl.when(z < LINE - 1)
            def _():
                to_right(m, LINE - 1).start()

            over(m, LINE - 1).start()

        @pl.when(z < LINE - 1)
        def _(m=m):
            arrived(m, 1)

            @pl.when(z > 0)
            def _():
                to_left(m, 1).start()

            over(m, 1).start()

    def fetch(m, rel, c):
        here = home(m, rel) if c == 0 else store.at[m, rel, 1]
        there = held.at[m, rel, c, pl.ds(0, height), :]
        return pltpu.make_async_copy(here, there, held_sem.at[m, rel, c])

    pieces = [(rel, c) for rel in range(LINE) for c in range(CORES)]
    share_of = LINE * CORES // n_tp

    def located(block):
        rel = lax.rem(block // CORES + LINE - z, LINE)
        c = jnp.where(lax.rem(block, CORES) == core, 0, 1)
        return rel, c, pl.ds(pl.multiple_of(block * width, width), width)

    def part_copy(step, d):
        at = pl.ds(pl.multiple_of(peers[d][1] * columns, columns), columns)
        return pltpu.make_async_remote_copy(
            parts.at[step, :, at], got.at[step, d], part_send.at[step, d], part_recv.at[step, d], peers[d], MESH
        )

    def square_copy(step, d):
        return pltpu.make_async_remote_copy(
            squares.at[step, n_tp - 1],
            squares.at[step, d],
            square_send.at[step, d],
            square_recv.at[step, d],
            peers[d],
            MESH,
        )

    results = [
        pltpu.make_async_copy(result.at[pl.ds(k * count, count), :], ref, back_sem.at[k])
        for k, ref in enumerate((mixed, outgoing))
    ]
    tail_out = pltpu.make_async_copy(
        held.at[EDGE, LINE // 2, 0, pl.ds(cut, height - cut), :], tail, back_sem.at[2]
    )
    both = 2 * count
    block = row_chunk(both, 32)
    tall = row_chunk(padded, 64)

    def second(m):
        arrived(m, 2)
        if m <= EDGE:
            at = early if m == EDGE else whole

            @pl.when(z == 1)
            def _():
                to_left(m, 2, at).start()

            @pl.when(z == 2)
            def _():
                to_right(m, 2, at).start()

        over(m, 2).start()

    @pl.when(outer)
    def _():
        for m in range(MATRICES):
            second(m)

    def ready(m):
        second(m)
        keep(m).wait()
        for rel in range(LINE):
            swapped(m, rel)
        for rel, c in pieces:
            fetch(m, rel, c).start()

    def fetched(m):
        for rel, c in pieces:
            fetch(m, rel, c).wait()

    @pl.when(inner)
    def _():
        for m in range(MATRICES):
            for rel, c in pieces:
                held[m, rel, c, pl.ds(height, padded - height), :] = jnp.zeros(
                    (padded - height, width), jnp.bfloat16
                )
        for step in range(2):
            gate_at, up_at, down_at = 3 * step, 3 * step + 1, 3 * step + 2
            ready(gate_at)
            ready(up_at)
            gate_sum[...] = jnp.zeros_like(gate_sum)
            up_sum[...] = jnp.zeros_like(up_sum)
            fetched(gate_at)
            fetched(up_at)
            total = jnp.zeros((1, both), jnp.float32)
            for d in range(-1, n_tp - 1):
                if d >= 0:
                    rows_in(step, d)
                source = sources[d] if d >= 0 else tp

                def gate_up(i, total, step=step, source=source, gate_at=gate_at, up_at=up_at):
                    rel, c, at = located(source * share_of + i)
                    flipped = rows[step, :, at].astype(jnp.float32).T
                    rhs = flipped.astype(jnp.bfloat16)
                    for m, product in ((gate_at, gate_sum), (up_at, up_sum)):
                        product[...] += jnp.dot(
                            held[m, rel, c], rhs, preferred_element_type=jnp.float32
                        )
                    return total + jnp.sum(flipped * flipped, axis=0, keepdims=True)

                total = lax.fori_loop(0, share_of, gate_up, total)
            scale = lax.rsqrt(total / features + norm_epsilon)

            def activate(i, _, scale=scale):
                at = pl.ds(pl.multiple_of(i * tall, 16), tall)
                gate = scale * gate_sum[at, :]
                hidden_turned[at, :] = gate / (1.0 + jnp.exp(-gate)) * (scale * up_sum[at, :])
                return 0

            lax.fori_loop(0, padded // tall, activate, 0)

            def turn_back(i, _):
                at = pl.ds(pl.multiple_of(i * LANES, LANES), LANES)
                hidden[:, at] = hidden_turned[at, :].T.astype(jnp.bfloat16)
                return 0

            lax.fori_loop(0, padded // LANES, turn_back, 0)
            ready(down_at)
            fetched(down_at)
            if down_at == EDGE:
                tail_out.start()
            for d in [*range(n_tp - 1), -1]:
                target = peers[d][1] if d >= 0 else tp

                def down(i, _, step=step, target=target, down_at=down_at):
                    rel, c, at = located(target * share_of + i)
                    parts[step, :, at] = jnp.dot(
                        hidden[...], held[down_at, rel, c], preferred_element_type=jnp.float32
                    ).astype(jnp.bfloat16)
                    return 0

                lax.fori_loop(0, share_of, down, 0)
                if d >= 0:
                    part_copy(step, d).start()
            for d in range(n_tp - 1):
                part_copy(step, d).wait_recv()

            def add_up(i, _, step=step):
                at = pl.ds(pl.multiple_of(i * block, 16), block)
                total = parts[step, at, mine_at].astype(jnp.float32)
                for d in range(n_tp - 1):
                    total = total + got[step, d, at, :].astype(jnp.float32)
                share[at, :] = total
                column[at, :] = jnp.broadcast_to(
                    jnp.sum(total * total, axis=1, keepdims=True), (block, LANES)
                )
                return 0

            lax.fori_loop(0, both // block, add_up, 0)
            squares[step, n_tp - 1] = column[...].T[:SUBLANES, :]
            for d in range(n_tp - 1):
                square_copy(step, d).start()
            for d in range(n_tp - 1):
                square_copy(step, d).wait_recv()
            square = squares[step, n_tp - 1]
            for d in range(n_tp - 1):
                square = square + squares[step, d]
            scale = lax.rsqrt(square[:1, :] / features + norm_epsilon)
            column[...] = jnp.broadcast_to(scale, (LANES, both)).T

            def finish(i, _, step=step):
                at = pl.ds(pl.multiple_of(i * block, 16), block)
                row = rows[step, at, mine_at].astype(jnp.float32)
                gain = posts[step][:, mine_at]
                out = (row + 0.5 * share[at, :] * column[at, :1] * gain).astype(jnp.bfloat16)
                if step == 0:
                    rows[1, at, mine_at] = out
                else:
                    result[at, :] = out
                return 0

            lax.fori_loop(0, both // block, finish, 0)
            if step == 0:
                for d in range(n_tp - 1):
                    row_copy(1, d).start()
        for copy in results:
            copy.start()

    @pl.when(outer)
    def _():
        for m in range(EDGE + 1):

            @pl.when(z == 0)
            def _(m=m):
                arrived_last(m, 3)
                if m < INNER:
                    over(m, 3).start()

            @pl.when(z == LINE - 1)
            def _(m=m):
                arrived_last(m, 1)
                if m < INNER:
                    over(m, 1).start()

        for m in range(MATRICES):
            keep(m).wait()
            swapped(m, 0)
            swapped(m, 2)

            @pl.when((z == 0) | (m < INNER))
            def _(m=m):
                swapped(m, 1)

            @pl.when((z == LINE - 1) | (m < INNER))
            def _(m=m):
                swapped(m, 3)

        token_in.wait_send()

    @pl.when(inner)
    def _():
        for copy in [*results, tail_out]:
            copy.wait()
        for step in range(2):
            for d in range(n_tp - 1):
                row_copy(step, d).wait_send()
                part_copy(step, d).wait_send()
                square_copy(step, d).wait_send()

    for m in range(MATRICES):
        over(m, 0).wait_send()
        over(m, 2).wait_send()

        @pl.when(z < LINE - 1)
        def _(m=m):
            to_right(m, 0).wait_send()
            over(m, 1).wait_send()

        @pl.when(z > 0)
        def _(m=m):
            to_left(m, 0).wait_send()
            over(m, 3).wait_send()

        @pl.when(inner)
        def _(m=m):
            to_right(m, 3).wait_send()
            to_left(m, 1).wait_send()

        if m <= EDGE:
            at = early if m == EDGE else whole

            @pl.when(z == 1)
            def _(m=m, at=at):
                to_left(m, 2, at).wait_send()

            @pl.when(z == 2)
            def _(m=m, at=at):
                to_right(m, 2, at).wait_send()

            if m < INNER:

                @pl.when(z == 0)
                def _(m=m):
                    over(m, 3).wait_send()

                @pl.when(z == LINE - 1)
                def _(m=m):
                    over(m, 1).wait_send()


def gather_and_mix(n_tp, tokens, gains, posts, weights):
    height, width = weights[0].shape
    count, columns = tokens.shape
    features = columns * n_tp
    both = 2 * count
    padded = pl.cdiv(height, LANES) * LANES
    cut = height // 2 // 16 * 16
    bf16, f32 = jnp.bfloat16, jnp.float32
    dma = pltpu.SemaphoreType.DMA
    others = n_tp - 1
    anywhere = pl.BlockSpec(memory_space=pl.ANY)
    vmem = pl.BlockSpec(memory_space=pltpu.VMEM)
    return pl.pallas_call(
        functools.partial(line_kernel, n_tp),
        out_shape=(
            jax.ShapeDtypeStruct((MATRICES, LINE, CORES, height, width), bf16),
            *(
                jax.ShapeDtypeStruct((extent, width), bf16)
                for extent in (height, 2 * height, height, height - cut, height + cut)
            ),
            *(jax.ShapeDtypeStruct((count, columns), bf16),) * 2,
        ),
        in_specs=[anywhere] + [vmem] * 4 + [anywhere] * MATRICES,
        out_specs=(anywhere,) * 8,
        scratch_shapes=[
            pltpu.VMEM((SLOTS, height, width), f32),
            pltpu.VMEM((MATRICES, height, width), bf16),
            pltpu.VMEM((MATRICES, LINE, CORES, padded, width), bf16),
            pltpu.VMEM((2, both, features), bf16),
            pltpu.VMEM((both, LANES), f32),
            pltpu.VMEM((padded, both), f32),
            pltpu.VMEM((padded, both), f32),
            pltpu.VMEM((padded, both), f32),
            pltpu.VMEM((both, padded), bf16),
            pltpu.VMEM((2, both, features), bf16),
            pltpu.VMEM((2, others, both, columns), bf16),
            pltpu.VMEM((both, columns), f32),
            pltpu.VMEM((2, n_tp, SUBLANES, both), f32),
            pltpu.VMEM((both, columns), bf16),
            pltpu.SemaphoreType.REGULAR,
            dma((MATRICES,)),
            dma((MATRICES,)),
            dma((MATRICES, LINE)),
            dma((MATRICES, LINE)),
            dma((MATRICES, LINE)),
            dma((MATRICES, LINE)),
            dma((MATRICES, LINE)),
            dma((MATRICES, LINE, CORES)),
            dma((3,)),
            dma((2, others)),
            dma((2, others)),
            dma((2, others)),
            dma((2, others)),
            dma((2, others)),
            dma((2, others)),
            dma((3,)),
        ],
        compiler_params=pltpu.CompilerParams(
            collective_id=0, has_side_effects=True, vmem_limit_bytes=63 << 20
        ),
        cost_estimate=pl.CostEstimate(
            flops=200_000_000_000, bytes_accessed=100_000_000, transcendentals=0
        ),
        name="gather_and_mix",
    )(tokens, *gains, *posts, *weights)


def place_kernel(slots, store, far_first, far_pair, far_last, mixed, *refs):
    outs, mixed_out = refs[:MATRICES], refs[MATRICES]
    held, small, in_sem, out_sem, small_sem = refs[MATRICES + 1 :]
    mixed_in = pltpu.make_async_copy(mixed, small, small_sem.at[0])
    mixed_on = pltpu.make_async_copy(small, mixed_out, small_sem.at[1])
    mixed_in.start()
    fs = lax.axis_index("fs")
    z, core = fs // CORES, lax.rem(fs, CORES)
    height, width = held.shape[1:]
    far = (
        far_first,
        far_pair.at[pl.ds(0, height)],
        far_pair.at[pl.ds(height, height)],
        far_last,
    )
    jobs = [(m, rel, c) for m in range(MATRICES) for rel in range(LINE) for c in range(CORES)]

    def if_here(i, act):
        m, rel, _ = jobs[i]
        if m < INNER or rel % 2 == 0:
            act()
        else:
            pl.when(z != (0 if rel == LINE - 1 else LINE - 1))(act)

    def take(i):
        m, rel, c = jobs[i]
        remote = rel == LINE // 2 and c == 0 and m >= EDGE
        piece = far[m - EDGE] if remote else store.at[m, rel, c]
        return pltpu.make_async_copy(piece, held.at[i % slots], in_sem.at[i % slots])

    def give(i):
        m, rel, c = jobs[i]
        source = lax.rem(z + rel, LINE) * CORES + (core if c == 0 else 1 - core)
        at = pl.ds(pl.multiple_of(source * width, width), width)
        return pltpu.make_async_copy(held.at[i % slots], outs[m].at[:, at], out_sem.at[i % slots])

    def pass_on(i):
        take(i).wait()
        give(i).start()

    lag = slots // 2
    for i in range(len(jobs) + lag):
        if i < len(jobs):
            if i >= slots:
                if_here(i - slots, lambda: give(i - slots).wait())
            if_here(i, lambda: take(i).start())
        if i == lag:
            mixed_in.wait()
            mixed_on.start()
        if i >= lag:
            if_here(i - lag, lambda: pass_on(i - lag))
    for i in range(len(jobs) - slots, len(jobs)):
        if_here(i, lambda: give(i).wait())
    mixed_on.wait()


def place(store, far, mixed):
    height, width = store.shape[3:]
    slots = 16
    anywhere = pl.BlockSpec(memory_space=pltpu.HBM)
    slab = jax.ShapeDtypeStruct((height, width * LINE * CORES), jnp.bfloat16)
    return pl.pallas_call(
        functools.partial(place_kernel, slots),
        out_shape=(slab,) * MATRICES + (jax.ShapeDtypeStruct(mixed.shape, mixed.dtype),),
        in_specs=[anywhere] * 5,
        out_specs=(anywhere,) * (MATRICES + 1),
        scratch_shapes=[
            pltpu.VMEM((slots, height, width), jnp.bfloat16),
            pltpu.VMEM(mixed.shape, mixed.dtype),
            pltpu.SemaphoreType.DMA((slots,)),
            pltpu.SemaphoreType.DMA((slots,)),
            pltpu.SemaphoreType.DMA((2,)),
        ],
        compiler_params=pltpu.CompilerParams(vmem_limit_bytes=62 << 20),
        cost_estimate=pl.CostEstimate(
            flops=20_000_000_000, bytes_accessed=68_000_000, transcendentals=0
        ),
        name="place",
    )(store, *far, mixed)


def put_kernel(spans, moves, *refs):
    n = len(spans)
    ins, refs = refs[n : n + 2 + 2 * moves], refs[n + 2 + 2 * moves :]
    slabs, refs = refs[:n], refs[n:]
    (mine, other), (held, sems) = ins[:2], refs[moves : moves + 2]
    fs = lax.axis_index("fs")
    z, core = fs // CORES, lax.rem(fs, CORES)
    width = mine.shape[1]
    copies = []
    for k, (start, extent, first) in enumerate(spans):
        for c, piece in enumerate((mine, other)):
            source = (LINE - 1 - z) * CORES + (core if c == 0 else 1 - core)
            at = pl.ds(pl.multiple_of(source * width, width), width)
            here = held.at[c, pl.ds(start, extent)]
            copies.append(
                (
                    pltpu.make_async_copy(piece.at[pl.ds(start, extent)], here, sems.at[k, c, 0]),
                    pltpu.make_async_copy(
                        here, slabs[k].at[pl.ds(first, extent), at], sems.at[k, c, 1]
                    ),
                )
            )

    if moves:
        small, small_sem = refs[moves + 2 :]
        copies.append(
            (
                pltpu.make_async_copy(ins[3], small, small_sem.at[0]),
                pltpu.make_async_copy(small, refs[0], small_sem.at[1]),
            )
        )

    @pl.when((z == 0) | (z == LINE - 1))
    def _():
        for take, _ in copies:
            take.start()
        for take, give in copies:
            take.wait()
            give.start()
        for _, give in copies:
            give.wait()


def put(slabs, mine, other, spans, replaced=()):
    anywhere = pl.BlockSpec(memory_space=pl.ANY)
    n, moves = len(slabs), len(replaced) // 2
    outs = [*slabs, *replaced[:moves]]
    scratch = [
        pltpu.VMEM((CORES, *mine.shape), mine.dtype),
        pltpu.SemaphoreType.DMA((n, CORES, 2)),
    ]
    if moves:
        scratch += [pltpu.VMEM(replaced[0].shape, replaced[0].dtype), pltpu.SemaphoreType.DMA((2,))]
    aliases = {k: k for k in range(n)} | {n + 2 + k: n + k for k in range(moves)}
    return pl.pallas_call(
        functools.partial(put_kernel, spans, moves),
        out_shape=tuple(jax.ShapeDtypeStruct(out.shape, out.dtype) for out in outs),
        in_specs=[anywhere] * (n + 2 + 2 * moves),
        out_specs=(anywhere,) * (n + moves),
        scratch_shapes=scratch,
        input_output_aliases=aliases,
        compiler_params=pltpu.CompilerParams(vmem_limit_bytes=8 << 20),
        cost_estimate=pl.CostEstimate(
            flops=1_000_000_000, bytes_accessed=3_000_000, transcendentals=0
        ),
        name="put",
    )(*slabs, mine, other, *replaced)


def hop(piece):
    pairs = [(a * CORES + c, b * CORES + c) for a, b in ((1, 0), (2, 3)) for c in range(CORES)]
    return lax.ppermute(piece, "fs", pairs)


def swap(piece):
    pairs = [(z * CORES + c, z * CORES + 1 - c) for z in (0, LINE - 1) for c in range(CORES)]
    return lax.ppermute(piece, "fs", pairs)


def line_program(n_tp):
    def on_device(
        tokens,
        first_gain,
        first_gate,
        first_up,
        first_down,
        first_post,
        second_gain,
        second_gate,
        second_up,
        second_down,
        second_post,
    ):
        gains = (first_gain[None, :], second_gain[None, :])
        posts = (first_post[None, :], second_post[None, :])
        weights = (first_gate.T, first_up.T, first_down, second_gate.T, second_up.T, second_down)
        outs = gather_and_mix(n_tp, tokens, gains, posts, weights)
        store, far, (tail, edge, mixed, outgoing) = outs[0], outs[1:4], outs[4:]
        height = far[0].shape[0]
        cut = edge.shape[0] - height
        moved = [hop(piece) for piece in (far[1], far[2], tail)]
        back = hop(outgoing)
        other = swap(edge)
        *slabs, mixed = place(store, far, mixed)
        ends = [
            ("edge", edge, (INNER, EDGE), ((0, height, 0), (height, cut, 0))),
            (0, moved[0], (EDGE + 1, EDGE + 2), ((0, height, 0), (height, height, 0))),
            (1, moved[1], (EDGE + 3,), ((0, height, 0),)),
            (2, moved[2], (EDGE,), ((0, height - cut, cut),)),
        ]
        for name, mine, at, spans in ends:
            if name != "edge":
                other = swap(mine)
            replaced = (mixed, back) if name == MOVES - 1 else ()
            placed = put([slabs[m] for m in at], mine, other, spans, replaced)
            for m, slab in zip(at, placed):
                slabs[m] = slab
        mixed = placed[-1]
        return (
            mixed,
            slabs[0].T,
            slabs[1].T,
            slabs[2],
            slabs[3].T,
            slabs[4].T,
            slabs[5],
        )

    return on_device


def ring_parts(block_of, n_tp):
    me = lax.axis_index("tp")
    got = [block_of(me)]
    for d in range(1, n_tp):
        move = [(i, (i + d) % n_tp) for i in range(n_tp)]
        got.append(lax.ppermute(block_of((me + d) % n_tp), "tp", move))
    return got


def all_columns(columns, n_tp):
    me = lax.axis_index("tp")
    width = columns.shape[1]
    if n_tp > 8:
        return lax.all_gather(columns, "tp", axis=1, tiled=True)
    full = jnp.zeros((columns.shape[0], width * n_tp), columns.dtype)
    for d, block in enumerate(ring_parts(lambda _: columns, n_tp)):
        start = ((me - d + n_tp) % n_tp) * width
        full = lax.dynamic_update_slice_in_dim(full, block, start, 1)
    return full


def hidden_of(full_rows, gate_slab, up_slab):
    rows_float = full_rows.astype(jnp.float32)
    scale = lax.rsqrt(jnp.mean(rows_float * rows_float, axis=1, keepdims=True) + norm_epsilon)
    gate = scale * jnp.dot(full_rows, gate_slab, preferred_element_type=jnp.float32)
    up = scale * jnp.dot(full_rows, up_slab, preferred_element_type=jnp.float32)
    return (jax.nn.silu(gate) * up).astype(jnp.bfloat16)


def finish(own_columns, parts, post, n_tp):
    width = own_columns.shape[1]
    me = lax.axis_index("tp")
    features = width * n_tp
    if n_tp > 8:
        share = lax.psum_scatter(parts, "tp", scatter_dimension=1, tiled=True).astype(jnp.float32)
        squares = lax.psum(jnp.sum(share * share, axis=1, keepdims=True), "tp")
    else:
        got = ring_parts(lambda to: lax.dynamic_slice_in_dim(parts, to * width, width, 1), n_tp)
        share = got[0].astype(jnp.float32)
        for part in got[1:]:
            share = share + part.astype(jnp.float32)
        own = jnp.sum(share * share, axis=1)[None, :]
        sums = ring_parts(lambda _: own, n_tp)
        squares = sums[0]
        for one in sums[1:]:
            squares = squares + one
        squares = squares.reshape(-1, 1)
    scale = lax.rsqrt(squares / features + norm_epsilon)
    gain_part = lax.dynamic_slice_in_dim(post, me * width, width, 0)
    return (own_columns.astype(jnp.float32) + 0.5 * share * scale * gain_part[None, :]).astype(
        jnp.bfloat16
    )


def gathered_program(n_tp):
    def on_device(
        tokens,
        first_gain,
        first_gate,
        first_up,
        first_down,
        first_post,
        second_gain,
        second_gate,
        second_up,
        second_down,
        second_post,
    ):
        pieces = half(first_gain, first_gate, first_up, first_down)
        pieces = pieces + half(second_gain, second_gate, second_up, second_down)
        slabs = [
            lax.all_gather(piece, "fs", axis=axis, tiled=True)
            for piece, axis in zip(pieces, (0, 0, 1) * 2)
        ]
        rows = tokens
        for (gate, up, down), post in ((slabs[:3], first_post), (slabs[3:], second_post)):
            parts = jnp.dot(
                hidden_of(all_columns(rows, n_tp), gate, up),
                down,
                preferred_element_type=jnp.float32,
            ).astype(jnp.bfloat16)
            rows = finish(rows, parts, post, n_tp)
        return (rows, *slabs)

    return on_device


def solution(mesh):
    chips, n_tp = mesh.shape["fs"] // CORES, mesh.shape["tp"]
    short = chips == LINE and LINE * CORES % n_tp == 0
    program = line_program(n_tp) if short else gathered_program(n_tp)

    placed = (
        P("fs", "tp"),
        P("fs"),
        P("fs", "tp"),
        P("fs", "tp"),
        P("tp", "fs"),
        P(),
        P("fs"),
        P("fs", "tp"),
        P("fs", "tp"),
        P("tp", "fs"),
        P(),
    )

    return jax.shard_map(
        program,
        mesh=mesh,
        in_specs=placed,
        out_specs=(
            P("fs", "tp"),
            P(None, "tp"),
            P(None, "tp"),
            P("tp", None),
            P(None, "tp"),
            P(None, "tp"),
            P("tp", None),
        ),
        check_vma=False,
    )
```
